32 devices in a mesh: kv: 4 (over y, x), tp: 8 (over z, core).
Axes of the slice: x: 2, y: 2, z: 4, core: 2. Of those that a mesh axis runs over, the one named last changes fastest.
Arguments:
- tokens: bfloat16 [3, 4096], P(None, ('kv', 'tp')), may hold values from -40 to 40
- lengths: int32 [3], replicated, may hold values from 1 to 8192, as said below
- attn_gain: float32 [4096], P(('kv', 'tp')), may hold values from 0.1 to 1.9
- w_query: bfloat16 [4096, 2048], P('kv', 'tp'), may hold values from -0.09375 to 0.09375
- w_key: bfloat16 [4096, 128], P('kv'), may hold values from -0.09375 to 0.09375
- w_value: bfloat16 [4096, 128], P('kv'), may hold values from -0.09375 to 0.09375
- w_forget: bfloat16 [4096, 32], replicated, may hold values from -0.09375 to 0.09375
- forget_bias: float32 [32], replicated, may hold values from -4 to 0
- cache_keys: bfloat16 [3, 128, 8192], P(None, None, ('kv', 'tp')), may hold values from -320 to 320
- cache_values: bfloat16 [3, 128, 8192], P(None, None, ('kv', 'tp')), may hold values from -6 to 6
- cache_decay: float32 [3, 32, 8192], P(None, None, ('kv', 'tp')), may hold values from -1028 to 0, as said below
- out_gain: float32 [2048], replicated, may hold values from 0.1 to 1.9
- w_out: bfloat16 [2048, 4096], P('tp', 'kv'), may hold values from -0.125 to 0.125
- mlp_gain: float32 [4096], P(('kv', 'tp')), may hold values from 0.1 to 1.9
- w_gate: bfloat16 [4096, 11264], P('kv', 'tp'), may hold values from -0.09375 to 0.09375
- w_up: bfloat16 [4096, 11264], P('kv', 'tp'), may hold values from -0.09375 to 0.09375
- w_down: bfloat16 [11264, 4096], P('tp', 'kv'), may hold values from -0.0546875 to 0.0546875
Outputs:
- layer_out: bfloat16 [3, 4096], P(None, ('kv', 'tp'))
The draws below stay inside these ranges and needn't reach their ends.
Inputs may be any that keep to these rules, and one draw needn't show every extreme that they name: Sequence b has lengths[b] live cache positions, 0 to lengths[b] - 1; some sequence has exactly 8192 in every draw. On live positions, cache_decay[b, h, j] is the sum of the log forget gates of sequence b and head h over positions j + 1 to lengths[b] - 1, so it is zero at the last live position and never rises toward earlier positions; it is zero beyond lengths[b].
All inputs are finite; a program needn't handle non-finite values.
Results may differ from the reference program's by a relative error of at most 0.013.
Values may be sent and summed in bfloat16 or wider, within the bound.
A program may use at most 64 MiB of HBM per device.

```python
import math
import jax
import jax.numpy as jnp
from jax import lax

D = 4096
QUERY_HEAD_COUNT = 32
HD = 64
KV_HEADS = 2
FF = 11264
SEQUENCE_COUNT = 3
LEN_DEV = 256
LEN = 8192
KV_COLS = 1024


def lengths_of(key):
    folded = jax.random.fold_in(key, 101)
    key_shift, key_cut, key_full = jax.random.split(folded, 3)
    shifts = jax.random.randint(key_shift, (SEQUENCE_COUNT,), 0, 6)
    longest = jnp.right_shift(jnp.full((SEQUENCE_COUNT,), LEN, jnp.int32), shifts)
    cut_off = jax.random.randint(key_cut, (SEQUENCE_COUNT,), 0, longest // 2 + 1)
    sequence_length = jnp.maximum(longest - cut_off, 1)
    chosen = jax.random.randint(key_full, (), 0, SEQUENCE_COUNT)
    return jnp.where(jnp.arange(SEQUENCE_COUNT) == chosen, LEN, sequence_length).astype(jnp.int32)


def draw_lengths(key, part):
    return lengths_of(key)


def draw_cache_decay(key, part):
    sequence_length = lengths_of(key)
    folded = jax.random.fold_in(key, 202)
    key_kind, key_block, key_rough, key_location, key_dimension = jax.random.split(folded, 5)
    lagging_heads = (jax.random.randint(key_kind, (QUERY_HEAD_COUNT,), 0, 2) == 1).astype(jnp.float32)
    base_rate = lagging_heads / LEN + (1.0 - lagging_heads) / 40.0
    log_two = math.log(2.0)
    blocks = LEN // LEN_DEV
    block_factor = jnp.exp(jax.random.uniform(key_block, (QUERY_HEAD_COUNT, blocks), jnp.float32, -log_two, log_two))
    block_factor = jnp.repeat(block_factor, LEN_DEV, axis=1)
    roughness = jnp.exp(jax.random.uniform(key_rough, (SEQUENCE_COUNT, QUERY_HEAD_COUNT, LEN), jnp.float32, -log_two, log_two))
    step_amount = base_rate[None, :, None] * block_factor[None] * roughness
    spike_locations = jax.random.randint(key_location, (SEQUENCE_COUNT, QUERY_HEAD_COUNT, 3), 0, sequence_length[:, None, None])
    spike_penalty = jax.random.uniform(key_dimension, (SEQUENCE_COUNT, QUERY_HEAD_COUNT, 3), jnp.float32, 0.2, 0.5)
    spike_offset = -jnp.log(1.0 - spike_penalty) * lagging_heads[None, :, None]
    token_positions = jnp.arange(LEN)
    for spike_index in range(3):
        match_found = token_positions[None, None, :] == spike_locations[:, :, spike_index:spike_index + 1]
        step_amount = step_amount + jnp.where(match_found, spike_offset[:, :, spike_index:spike_index + 1], 0.0)
    running = jnp.cumsum(step_amount, axis=2)
    newest = jnp.broadcast_to((sequence_length - 1)[:, None, None], (SEQUENCE_COUNT, QUERY_HEAD_COUNT, 1))
    at_newest = jnp.take_along_axis(running, newest, axis=2)
    return jnp.where(token_positions[None, None, :] < sequence_length[:, None, None], running - at_newest, 0.0).astype(jnp.float32)


def draw_cache_keys(key, part):
    folded = jax.random.fold_in(key, 303)
    key_base = jax.random.fold_in(folded, 0)
    full_shape = (SEQUENCE_COUNT, KV_HEADS, HD, LEN)
    entries = jnp.clip(jax.random.normal(key_base, full_shape, jnp.float32), -6.0, 6.0)
    return entries.reshape(SEQUENCE_COUNT, KV_HEADS * HD, LEN).astype(jnp.bfloat16)


def draw_tokens(key, part):
    folded = jax.random.fold_in(key, 404)
    key_value = jax.random.fold_in(folded, 0)
    column = jnp.arange(D)
    inside = (column % KV_COLS).astype(jnp.float32) / KV_COLS
    log_three = math.log(3.0)
    column_scale = 0.4 * jnp.exp(log_three * column.astype(jnp.float32) / D + log_three * inside)
    entries = jnp.clip(jax.random.normal(key_value, (SEQUENCE_COUNT, D), jnp.float32), -6.0, 6.0)
    return (entries * column_scale[None, :]).astype(jnp.bfloat16)


def shard_levels(stream_key, dims, cuts, least, largest):
    def one(dim, shards_of):
        heights = jax.random.uniform(jax.random.fold_in(jax.random.fold_in(stream_key, 6), dim), (shards_of,), jnp.float32, least / len(cuts), largest / len(cuts))
        return jnp.repeat(jnp.exp(heights), dims[dim] // shards_of).reshape((-1,) + (1,) * (len(dims) - dim - 1))

    gain = one(*cuts[0])
    for cut in cuts[1:]:
        gain = gain * one(*cut)
    return gain


def noise(stream_key, shape, width, limit, cuts=(), kind=jnp.bfloat16):
    factor_of = shard_levels(stream_key, shape, cuts, -0.22, 0.18) if cuts else 1.0
    result = jax.random.normal(stream_key, shape, jnp.float32) * width * factor_of
    return jnp.minimum(jnp.maximum(result, -limit), limit).astype(kind)


def setup_inputs(seed: int = 0) -> dict:
    seeds = jax.random.split(jax.random.key(seed), 18)
    return {
        "tokens": draw_tokens(jax.random.fold_in(seeds[17], 71), 0),
        "lengths": draw_lengths(jax.random.fold_in(seeds[17], 71), 0),
        "attn_gain": jnp.clip(1.0 + 0.18 * jax.random.normal(seeds[2], (D,), jnp.float32), 0.1, 1.9),
        "w_query": noise(seeds[3], (D, QUERY_HEAD_COUNT * HD), D ** -0.5, 0.09375, ((0, 4), (1, 8))),
        "w_key": noise(seeds[4], (D, KV_HEADS * HD), D ** -0.5, 0.09375, ((0, 4),)),
        "w_value": noise(seeds[5], (D, KV_HEADS * HD), D ** -0.5, 0.09375, ((0, 4),)),
        "w_forget": noise(seeds[6], (D, QUERY_HEAD_COUNT), D ** -0.5, 0.09375),
        "forget_bias": jnp.clip(jax.random.uniform(seeds[7], (QUERY_HEAD_COUNT,), jnp.float32, -4.0, 0.0), -4.0, 0.0),
        "cache_keys": draw_cache_keys(jax.random.fold_in(seeds[17], 71), 0),
        "cache_values": noise(seeds[9], (SEQUENCE_COUNT, KV_HEADS * HD, LEN), 1.0, 6.0, ((2, 32),)),
        "cache_decay": draw_cache_decay(jax.random.fold_in(seeds[17], 71), 0),
        "out_gain": jnp.clip(1.0 + 0.18 * jax.random.normal(seeds[11], (QUERY_HEAD_COUNT * HD,), jnp.float32), 0.1, 1.9),
        "w_out": noise(seeds[12], (QUERY_HEAD_COUNT * HD, D), (QUERY_HEAD_COUNT * HD) ** -0.5, 0.125, ((0, 8), (1, 4))),
        "mlp_gain": jnp.clip(1.0 + 0.18 * jax.random.normal(seeds[13], (D,), jnp.float32), 0.1, 1.9),
        "w_gate": noise(seeds[14], (D, FF), D ** -0.5, 0.09375, ((0, 4), (1, 8))),
        "w_up": noise(seeds[15], (D, FF), D ** -0.5, 0.09375, ((0, 4), (1, 8))),
        "w_down": noise(seeds[16], (FF, D), FF ** -0.5, 0.0546875, ((0, 8), (1, 4))),
    }


epsilon = 1e-06
masked_score = -1e+30

def inverse_rms(rows):
    values = rows.astype(jnp.float32)
    return lax.rsqrt(lax.optimization_barrier(jnp.mean(values * values, axis=1, keepdims=True)) + epsilon)

def attend_sequence(items):
    query_row, key_row, value_row, keys_seq, values_seq, decay_seq, gate_row, length_one = items
    groups = QUERY_HEAD_COUNT // KV_HEADS
    score_scale = HD ** (-0.5)
    query_grouped = query_row.astype(jnp.float32).reshape(KV_HEADS, groups, HD)
    keys_grouped = keys_seq.astype(jnp.float32).reshape(KV_HEADS, HD, LEN)
    values_grouped = values_seq.astype(jnp.float32).reshape(KV_HEADS, HD, LEN)
    scores = jnp.einsum('kgd,kdj->kgj', query_grouped, keys_grouped).reshape(QUERY_HEAD_COUNT, LEN)
    scores = scores * score_scale + decay_seq + gate_row[:, None]
    is_live = (jnp.arange(LEN, dtype=jnp.int32) < length_one)[None, :]
    scores = jnp.where(is_live, scores, masked_score)
    own_score = jnp.einsum('kgd,kd->kg', query_grouped, key_row.astype(jnp.float32).reshape(KV_HEADS, HD)).reshape(QUERY_HEAD_COUNT) * score_scale
    score_top = jnp.maximum(lax.optimization_barrier(jnp.max(scores, axis=1)), own_score)
    weights = jnp.where(is_live, jnp.exp(scores - score_top[:, None]), 0.0)
    own_weight = jnp.exp(own_score - score_top)
    weight_total = lax.optimization_barrier(jnp.sum(weights, axis=1)) + own_weight
    rounded = lax.optimization_barrier(weights.astype(jnp.bfloat16)).astype(jnp.float32)
    value_sums = jnp.einsum('kgj,kdj->kgd', rounded.reshape(KV_HEADS, groups, LEN), values_grouped).reshape(QUERY_HEAD_COUNT, HD)
    new_values = jnp.repeat(value_row.astype(jnp.float32).reshape(KV_HEADS, HD), groups, axis=0)
    value_sums = value_sums + own_weight[:, None] * new_values
    return value_sums / weight_total[:, None]

def reference(tokens, lengths, attn_gain, w_query, w_key, w_value, w_forget, forget_bias, cache_keys, cache_values, cache_decay, out_gain, w_out, mlp_gain, w_gate, w_up, w_down):
    batch_rows = tokens.shape[0]
    first_rms = inverse_rms(tokens)
    scaled_one = (tokens.astype(jnp.float32) * attn_gain).astype(jnp.bfloat16)
    query = (jnp.dot(scaled_one, w_query, preferred_element_type=jnp.float32) * first_rms).astype(jnp.bfloat16)
    key_new = (jnp.dot(scaled_one, w_key, preferred_element_type=jnp.float32) * first_rms).astype(jnp.bfloat16)
    value_new = (jnp.dot(scaled_one, w_value, preferred_element_type=jnp.float32) * first_rms).astype(jnp.bfloat16)
    log_gate = jax.nn.log_sigmoid(jnp.dot(scaled_one, w_forget, preferred_element_type=jnp.float32) * first_rms + forget_bias)
    heads_out = lax.map(attend_sequence, (query, key_new, value_new, cache_keys, cache_values, cache_decay, log_gate, lengths))
    normed = heads_out * lax.rsqrt(lax.optimization_barrier(jnp.mean(heads_out * heads_out, axis=2, keepdims=True)) + epsilon) * out_gain.reshape(QUERY_HEAD_COUNT, HD)
    normed = normed.astype(jnp.bfloat16).reshape(batch_rows, QUERY_HEAD_COUNT * HD)
    residual = (tokens.astype(jnp.float32) + jnp.dot(normed, w_out, preferred_element_type=jnp.float32)).astype(jnp.bfloat16)
    second_rms = inverse_rms(residual)
    scaled_two = (residual.astype(jnp.float32) * mlp_gain).astype(jnp.bfloat16)
    gate = jnp.dot(scaled_two, w_gate, preferred_element_type=jnp.float32) * second_rms
    up_part = jnp.dot(scaled_two, w_up, preferred_element_type=jnp.float32) * second_rms
    hidden = (jax.nn.silu(gate) * up_part).astype(jnp.bfloat16)
    return (residual.astype(jnp.float32) + jnp.dot(hidden, w_down, preferred_element_type=jnp.float32)).astype(jnp.bfloat16)
```

```python
import functools

import jax
import jax.numpy as jnp
from jax import lax
from jax.experimental import pallas as pl
from jax.experimental.pallas import tpu as pltpu
from jax.sharding import PartitionSpec as P

QUERY_HEAD_COUNT = 32
HD = 64
KV_HEADS = 2


epsilon = 1e-06
masked_score = -1e30


def spread_rows(share, gain):
    scaled = (share.astype(jnp.float32) * gain).astype(jnp.bfloat16)
    squares = jnp.sum(jnp.square(share.astype(jnp.float32)), axis=1)
    row_block = lax.all_gather(scaled, "tp", axis=1, tiled=True)
    square_total = lax.psum(squares, ("kv", "tp"))
    return (row_block, square_total)


def body(
    tokens,
    lengths,
    attn_gain,
    w_query,
    w_key,
    w_value,
    w_forget,
    forget_bias,
    cache_keys,
    cache_values,
    cache_decay,
    out_gain,
    w_out,
    mlp_gain,
    w_gate,
    w_up,
    w_down,
):
    full_width = tokens.shape[1] * lax.axis_size("kv") * lax.axis_size("tp")
    kv_index = lax.axis_index("kv")
    tp_index = lax.axis_index("tp")
    row_block, square_total = spread_rows(tokens, attn_gain)
    block_rows = row_block.shape[1]
    forget_rows = lax.dynamic_slice_in_dim(w_forget, kv_index * block_rows, block_rows, 0)
    query_part = jnp.dot(row_block, w_query, preferred_element_type=jnp.float32)
    key_part = jnp.dot(row_block, w_key, preferred_element_type=jnp.float32)
    value_part = jnp.dot(row_block, w_value, preferred_element_type=jnp.float32)
    forget_part = jnp.dot(row_block, forget_rows, preferred_element_type=jnp.float32)
    query_sum, key_sum, value_sum, forget_sum = lax.psum(
        (query_part, key_part, value_part, forget_part), "kv"
    )
    first_rms = lax.rsqrt(square_total / full_width + epsilon)[:, None]
    query_local = (query_sum * first_rms).astype(jnp.bfloat16)
    key_new = (key_sum * first_rms).astype(jnp.bfloat16)
    value_new = (value_sum * first_rms).astype(jnp.bfloat16)
    log_gate = jax.nn.log_sigmoid(forget_sum * first_rms + forget_bias)
    query_all = lax.all_gather(query_local, "tp", axis=1, tiled=True)
    batch_rows, key_dims, span = cache_keys.shape
    groups = QUERY_HEAD_COUNT // KV_HEADS
    score_scale = HD ** (-0.5)
    query_grouped = query_all.reshape(batch_rows, KV_HEADS, groups, HD)
    keys_grouped = cache_keys.reshape(batch_rows, KV_HEADS, HD, span)
    values_grouped = cache_values.reshape(batch_rows, KV_HEADS, HD, span)
    scores = jnp.einsum(
        "bkgd,bkdj->bkgj", query_grouped, keys_grouped, preferred_element_type=jnp.float32
    ).reshape(batch_rows, QUERY_HEAD_COUNT, span)
    scores = scores * score_scale + cache_decay + log_gate[:, :, None]
    first_slot = (kv_index * lax.axis_size("tp") + tp_index) * span
    token_positions = first_slot + lax.iota(jnp.int32, span)
    is_live = (token_positions[None, :] < lengths[:, None])[:, None, :]
    scores = jnp.where(is_live, scores, masked_score)
    own_score = (
        jnp.einsum(
            "inpo,ino->inp",
            query_grouped,
            key_new.reshape(batch_rows, KV_HEADS, HD),
            preferred_element_type=jnp.float32,
        ).reshape(batch_rows, QUERY_HEAD_COUNT)
        * score_scale
    )
    local_top = jnp.maximum(jnp.max(scores, axis=2), own_score)
    head_count = w_out.shape[0] // HD
    head_start = tp_index * head_count
    score_top = lax.pmax(local_top, ("kv", "tp"))
    weights = jnp.where(is_live, jnp.exp(scores - score_top[:, :, None]), 0.0)
    weight_total = jnp.sum(weights, axis=2)
    rounded = weights.astype(jnp.bfloat16).reshape(batch_rows, KV_HEADS, groups, span)
    value_sums = jnp.einsum(
        "bkgj,bkdj->bkgd", rounded, values_grouped, preferred_element_type=jnp.float32
    ).reshape(batch_rows, QUERY_HEAD_COUNT, HD)
    weight_total, value_sums = (weight_total, value_sums)
    weight_total, value_sums = (
        lax.psum_scatter(weight_total, "tp", scatter_dimension=1, tiled=True),
        lax.psum_scatter(value_sums, "tp", scatter_dimension=1, tiled=True),
    )
    weight_total, value_sums = lax.psum((weight_total, value_sums), "kv")
    score_top = lax.dynamic_slice_in_dim(score_top, head_start, head_count, 1)
    own_here = lax.dynamic_slice_in_dim(own_score, head_start, head_count, 1)
    new_values = jnp.repeat(value_new.reshape(batch_rows, KV_HEADS, HD), groups, axis=1)
    new_values = lax.dynamic_slice_in_dim(new_values, head_start, head_count, 1).astype(jnp.float32)
    own_weight = jnp.exp(own_here - score_top)
    heads_out = (value_sums + own_weight[:, :, None] * new_values) / (weight_total + own_weight)[
        :, :, None
    ]
    head_gains = lax.dynamic_slice_in_dim(out_gain, head_start * HD, head_count * HD, 0).reshape(
        head_count, HD
    )
    normed = (
        heads_out
        * lax.rsqrt(jnp.mean(jnp.square(heads_out), axis=2, keepdims=True) + epsilon)
        * head_gains
    )
    normed = normed.astype(jnp.bfloat16).reshape(batch_rows, head_count * HD)
    attn_part = jnp.dot(normed, w_out, preferred_element_type=jnp.float32)
    attn_share = lax.psum_scatter(attn_part, "tp", scatter_dimension=1, tiled=True)
    residual = (tokens.astype(jnp.float32) + attn_share).astype(jnp.bfloat16)
    mlp_block, mlp_squares = spread_rows(residual, mlp_gain)
    gate_part = jnp.dot(mlp_block, w_gate, preferred_element_type=jnp.float32)
    up_part = jnp.dot(mlp_block, w_up, preferred_element_type=jnp.float32)
    gate_sum, up_sum = lax.psum((gate_part, up_part), "kv")
    second_rms = lax.rsqrt(mlp_squares / full_width + epsilon)[:, None]
    hidden = (jax.nn.silu(gate_sum * second_rms) * (up_sum * second_rms)).astype(jnp.bfloat16)
    down_part = jnp.dot(hidden, w_down, preferred_element_type=jnp.float32)
    mlp_share = lax.psum_scatter(down_part, "tp", scatter_dimension=1, tiled=True)
    return (residual.astype(jnp.float32) + mlp_share).astype(jnp.bfloat16)


LANES = 128
ROWS = 8
MESH = pl.DeviceIdType.MESH


def column_chunks(columns):
    first = (columns // LANES + 1) // 2 * LANES
    return ((0, first), (first, columns))


def exchange(buffer, mine, axis, count, send_sems, recv_sems, source=None):
    copies = []
    for step in range(1, count):
        partner = lax.rem(mine + step, count)
        copy = pltpu.make_async_remote_copy(
            src_ref=buffer.at[mine] if source is None else source(partner),
            dst_ref=buffer.at[mine],
            send_sem=send_sems.at[step - 1],
            recv_sem=recv_sems.at[step - 1],
            device_id={axis: partner},
            device_id_type=MESH,
        )
        copy.start()
        copies.append(copy)
    return copies


def arrive(copies):
    for copy in copies:
        copy.wait_recv()


def merge_partials(buffer, count, lane):
    parts = [buffer[i] for i in range(count)]
    tops = [part[:, HD : HD + 1] for part in parts]
    top = functools.reduce(jnp.maximum, tops)
    total = functools.reduce(
        jnp.add, [jnp.exp(one - top) * part for one, part in zip(tops, parts)]
    )
    return jnp.where((lane >= HD) & (lane < HD + HD // 2), top, total)


def layer_kernel(
    kv_count,
    tp_count,
    lengths,
    tokens,
    attn_gain,
    mlp_gain,
    forget_bias,
    out_gain,
    w_query_hbm,
    w_key_hbm,
    w_value_hbm,
    w_forget_hbm,
    keys_hbm,
    values_hbm,
    decay_hbm,
    w_out_hbm,
    w_gate_hbm,
    w_up_hbm,
    w_down_hbm,
    out,
    w_query,
    w_key,
    w_value,
    w_forget,
    keys,
    values,
    decay,
    w_out,
    w_gate,
    w_up,
    w_down,
    token_buf,
    proj_buf,
    query_buf,
    part_send,
    part_buf,
    merged_buf,
    normed_buf,
    attn_buf,
    residual_buf,
    square_buf,
    gate_buf0,
    gate_buf1,
    down_send,
    down_buf,
    local_sem,
    tp_send,
    tp_recv,
    kv_send,
    kv_recv,
):
    kv = lax.axis_index("kv")
    tp = lax.axis_index("tp")
    batch = tokens.shape[0]
    half = ROWS // 2
    width = tokens.shape[1] * kv_count * tp_count
    block = w_query.shape[0]
    span = keys.shape[2]
    f32, bf16 = jnp.float32, jnp.bfloat16

    loads = {}

    def load(name, source, target):
        copy = pltpu.make_async_copy(source, target, local_sem.at[len(loads)])
        copy.start()
        loads[name] = copy

    load("query", w_query_hbm, w_query)
    load("key", w_key_hbm, w_key)
    load("value", w_value_hbm, w_value)
    load("forget", w_forget_hbm.at[pl.ds(pl.multiple_of(kv * block, block), block), :], w_forget)

    barrier = pltpu.get_barrier_semaphore()
    for step in range(1, tp_count):
        pl.semaphore_signal(
            barrier, inc=1, device_id={"tp": lax.rem(tp + step, tp_count)}, device_id_type=MESH
        )
    for step in range(1, kv_count):
        pl.semaphore_signal(
            barrier, inc=1, device_id={"kv": lax.rem(kv + step, kv_count)}, device_id_type=MESH
        )
    token_buf[tp, 0:batch, :] = tokens[...].astype(f32)
    token_buf[tp, batch : batch + 1, :] = attn_gain[...]
    token_buf[tp, batch + 1 : batch + 2, :] = mlp_gain[...]
    token_buf[tp, batch + 2 : ROWS, :] = jnp.zeros((ROWS - batch - 2, LANES), f32)
    pl.semaphore_wait(barrier, tp_count + kv_count - 2)

    pending = []

    def tp_exchange(index, buffer, source=None):
        copies = exchange(
            buffer, tp, "tp", tp_count, tp_send.at[index], tp_recv.at[index], source
        )
        pending.extend(copies)
        return copies

    def kv_exchange(index, buffer):
        copies = exchange(buffer, kv, "kv", kv_count, kv_send.at[index], kv_recv.at[index])
        pending.extend(copies)
        return copies

    token_copies = tp_exchange(0, token_buf)
    load("keys", keys_hbm, keys)
    for c in range(span // LANES):
        load("decay%d" % c, decay_hbm.at[:, :, pl.ds(c * LANES, LANES)], decay.at[c])
    load("values", values_hbm, values)
    load("out", w_out_hbm, w_out)
    load("gate", w_gate_hbm, w_gate)
    load("up", w_up_hbm, w_up)
    load("down", w_down_hbm, w_down)
    part_send[...] = jnp.zeros(part_send.shape, f32)
    down_send[...] = jnp.zeros(down_send.shape, f32)

    arrive(token_copies)
    blocks = [token_buf[i] for i in range(tp_count)]
    scaled = jnp.concatenate([b * b[batch : batch + 1, :] for b in blocks], axis=1).astype(bf16)
    squares = functools.reduce(jnp.add, [b * b for b in blocks])
    squares = jnp.sum(squares, axis=1, keepdims=True)
    loads["query"].wait()
    query = jnp.dot(scaled, w_query[...], preferred_element_type=f32)
    loads["key"].wait()
    key = jnp.dot(scaled, w_key[...], preferred_element_type=f32)
    loads["value"].wait()
    value = jnp.dot(scaled, w_value[...], preferred_element_type=f32)
    loads["forget"].wait()
    forget = jnp.dot(scaled, w_forget[...], preferred_element_type=f32)
    proj_buf[kv, 0] = jnp.concatenate([query[:half, :LANES], query[:half, LANES:]], axis=0)
    proj_buf[kv, 1] = jnp.concatenate([key[:half], value[:half]], axis=0)
    heads = forget.shape[1]
    proj_buf[kv, 2, :, 0:heads] = forget
    proj_buf[kv, 2, :, heads:LANES] = jnp.broadcast_to(squares, (ROWS, LANES - heads))
    arrive(kv_exchange(0, proj_buf))
    sums = [
        functools.reduce(jnp.add, [proj_buf[i, piece] for i in range(kv_count)])
        for piece in range(3)
    ]
    rms = lax.rsqrt(sums[2][:, heads : heads + 1] / width + epsilon)
    rms_twice = jnp.concatenate([rms[:half], rms[:half]], axis=0)
    query_rows = pl.ds(pl.multiple_of(tp * ROWS, ROWS), ROWS)
    query_buf[tp] = (sums[0] * rms_twice).astype(bf16).astype(f32)
    query_copies = tp_exchange(1, query_buf)
    new_rows = (sums[1] * rms_twice).astype(bf16).astype(f32)
    raw_gate = sums[2][:, 0:heads] * rms + forget_bias[...]
    log_gate = jnp.minimum(raw_gate, 0.0) - jnp.log1p(jnp.exp(-jnp.abs(raw_gate)))

    lane = lax.broadcasted_iota(jnp.int32, (ROWS, LANES), 1)
    group_rows = heads // KV_HEADS
    row_id = lax.broadcasted_iota(jnp.int32, (heads, heads), 0)
    row_rest = row_id % group_rows
    head_of_row = (
        row_id // group_rows * group_rows + row_rest % (group_rows // 2) * 2
        + row_rest // (group_rows // 2)
    )
    head_pick = head_of_row == lax.broadcasted_iota(jnp.int32, (heads, heads), 1)
    slots = lax.broadcasted_iota(jnp.int32, (heads, span), 1)
    slots = slots + (kv * tp_count + tp) * span
    first_device = jnp.broadcast_to(kv * tp_count + tp, (heads, 1)) == 0
    score_scale = HD ** (-0.5)
    arrive(query_copies)
    query_flat = query_buf.reshape(tp_count * ROWS, LANES)
    half_rows = group_rows // 2
    pairs = [(g, p) for g in range(KV_HEADS) for p in range(2)]
    loads["keys"].wait()
    loads["values"].wait()
    for c in range(span // LANES):
        loads["decay%d" % c].wait()
    for b in range(batch):
        pieces = []
        for g, p in pairs:
            rows = query_flat[pl.ds(g * half_rows * half + b, half_rows, stride=half), :]
            if p != g:
                rows = pltpu.roll(rows, HD, 1)
            pieces.append(jnp.where(lane // HD == g, rows, 0.0))
        queries = jnp.concatenate(pieces, axis=0)
        own = jnp.sum(queries * new_rows[b : b + 1, :], axis=1, keepdims=True) * score_scale
        scores = jnp.dot(queries.astype(bf16), keys[b], preferred_element_type=f32)
        faded = jnp.concatenate(
            [
                jnp.concatenate(
                    [
                        decay[c, b, pl.ds(g * group_rows + p, half_rows, stride=2), :]
                        for g, p in pairs
                    ],
                    axis=0,
                )
                for c in range(span // LANES)
            ],
            axis=1,
        )
        gate_rows = jnp.sum(
            jnp.where(head_pick, log_gate[b : b + 1, :], 0.0), axis=1, keepdims=True
        )
        live = slots < lengths[b]
        scores = jnp.where(live, scores * score_scale + faded + gate_rows, masked_score)
        top = jnp.max(scores, axis=1, keepdims=True)
        top = jnp.where(first_device, jnp.maximum(top, own), top)
        weights = jnp.where(live, jnp.exp(scores - top), 0.0)
        own_weight = jnp.where(first_device, jnp.exp(jnp.minimum(own - top, 0.0)), 0.0)
        total = jnp.sum(weights, axis=1, keepdims=True) + own_weight
        mixed = lax.dot_general(
            weights.astype(bf16),
            values[b],
            (((1,), (1,)), ((), ())),
            preferred_element_type=f32,
        )
        mixed = mixed + own_weight * new_rows[half + b : half + b + 1, :]
        for i, (g, p) in enumerate(pairs):
            rows = slice(i * half_rows, (i + 1) * half_rows)
            tile = mixed[rows]
            if g:
                tile = pltpu.roll(tile, HD, 1)
            tile = jnp.where(
                lane < HD, tile, jnp.where(lane < HD + HD // 2, top[rows], total[rows])
            )
            part_send[pl.ds(g * half_rows * ROWS + 2 * b + p, half_rows, stride=ROWS), :] = tile

    def part_of(index):
        return pl.ds(pl.multiple_of(index * 2 * ROWS, 2 * ROWS), 2 * ROWS)

    part_copies = tp_exchange(2, part_buf, lambda partner: part_send.at[part_of(partner), :])
    part_buf[tp] = part_send[part_of(tp), :]
    lane2 = lax.broadcasted_iota(jnp.int32, (2 * ROWS, LANES), 1)
    row2 = lax.broadcasted_iota(jnp.int32, (2 * ROWS, LANES), 0)
    gain_row = lax.broadcasted_iota(jnp.int32, out_gain.shape, 0)
    gain_tiles = []
    for j in range(2):
        gain = jnp.sum(
            jnp.where(gain_row == 2 * tp + j, out_gain[...], 0.0), axis=0, keepdims=True
        )
        gain = jnp.broadcast_to(gain, (ROWS, LANES))
        gain_tiles.append(jnp.where(row2[:ROWS] % 2 == 0, gain, pltpu.roll(gain, HD, 1)))
    gains = jnp.concatenate(gain_tiles, axis=0)
    arrive(part_copies)
    merged_buf[kv] = merge_partials(part_buf, tp_count, lane2)
    arrive(kv_exchange(1, merged_buf))
    merged = merge_partials(merged_buf, kv_count, lane2)
    total = merged[:, HD + HD // 2 : HD + HD // 2 + 1]
    total = jnp.where(row2[:, 0:1] % ROWS < 2 * batch, total, 1.0)
    heads_out = jnp.where(lane2 < HD, merged / total, 0.0)
    mean = jnp.sum(heads_out * heads_out, axis=1, keepdims=True) / HD
    normed_buf[...] = heads_out * lax.rsqrt(mean + epsilon) * gains
    columns = []
    for j in range(2):
        even = normed_buf[pl.ds(j * ROWS, half, stride=2), :]
        odd = normed_buf[pl.ds(j * ROWS + 1, half, stride=2), :]
        columns.append(jnp.where(lane[:half] < HD, even, pltpu.roll(odd, HD, 1)))
    normed = jnp.concatenate(columns, axis=1).astype(bf16)

    loads["out"].wait()
    attn = jnp.dot(normed, w_out[...], preferred_element_type=f32)
    middle = attn.shape[1] // 2
    attn_buf[tp] = jnp.concatenate([attn[:, :middle], attn[:, middle:]], axis=0).astype(bf16)
    arrive(tp_exchange(3, attn_buf))
    attn = functools.reduce(jnp.add, [attn_buf[i].astype(f32) for i in range(tp_count)])
    attn = jnp.concatenate([attn[:half], attn[half:]], axis=1)
    token_rows = jnp.concatenate([token_buf[i][:half] for i in range(tp_count)], axis=1)
    residual = (token_rows + attn).astype(bf16).astype(f32)
    squares = jnp.sum(residual * residual, axis=1, keepdims=True)
    square_buf[kv] = jnp.broadcast_to(
        jnp.concatenate([squares, squares], axis=0), (ROWS, LANES)
    )
    square_copies = kv_exchange(2, square_buf)
    for i in range(tp_count):
        residual_buf[i, 0:half, :] = residual[:, i * LANES : (i + 1) * LANES]
    gain_rows = jnp.concatenate(
        [token_buf[i][batch + 1 : batch + 2] for i in range(tp_count)], axis=1
    )
    scaled = (residual * gain_rows).astype(bf16)

    loads["gate"].wait()
    loads["up"].wait()
    chunks = column_chunks(w_gate.shape[1])
    gate_bufs = (gate_buf0, gate_buf1)
    gate_copies = []
    for index, (begin, end) in enumerate(chunks):
        gate = jnp.dot(scaled, w_gate[:, begin:end], preferred_element_type=f32)
        up = jnp.dot(scaled, w_up[:, begin:end], preferred_element_type=f32)
        gate_bufs[index][kv] = jnp.concatenate([gate, up], axis=0).astype(bf16)
        gate_copies.append(kv_exchange(3 + index, gate_bufs[index]))
    arrive(square_copies)
    squares = functools.reduce(jnp.add, [square_buf[i] for i in range(kv_count)])
    rms = lax.rsqrt(squares[:half, 0:1] / width + epsilon)
    loads["down"].wait()
    down = jnp.zeros((half, w_down.shape[1]), f32)
    for index, (begin, end) in enumerate(chunks):
        arrive(gate_copies[index])
        both = functools.reduce(
            jnp.add, [gate_bufs[index][i].astype(f32) for i in range(kv_count)]
        )
        gate, up = both[:half] * rms, both[half:] * rms
        hidden = (gate / (1.0 + jnp.exp(-gate)) * up).astype(bf16)
        down = down + jnp.dot(hidden, w_down[begin:end, :], preferred_element_type=f32)
    for i in range(tp_count):
        down_send[i, 0:half, :] = down[:, i * LANES : (i + 1) * LANES]
    down_copies = tp_exchange(4, down_buf, lambda partner: down_send.at[partner])
    down_buf[tp] = down_send[tp]
    arrive(down_copies)
    share = functools.reduce(jnp.add, [down_buf[i] for i in range(tp_count)])
    final = residual_buf[tp][0:batch] + share[0:batch]
    out[...] = final.astype(bf16)
    for copy in pending:
        copy.wait_send()


def kernel_layer(
    kv_count,
    tp_count,
    tokens,
    lengths,
    attn_gain,
    w_query,
    w_key,
    w_value,
    w_forget,
    forget_bias,
    cache_keys,
    cache_values,
    cache_decay,
    out_gain,
    w_out,
    mlp_gain,
    w_gate,
    w_up,
    w_down,
):
    f32, bf16 = jnp.float32, jnp.bfloat16
    batch, _, span = cache_keys.shape
    heads = w_forget.shape[1]
    block = w_query.shape[0]
    columns = w_out.shape[1]
    chunks = column_chunks(w_gate.shape[1])
    in_vmem = pl.BlockSpec(memory_space=pltpu.VMEM)
    anywhere = pl.BlockSpec(memory_space=pl.ANY)
    chunk_count = span // LANES
    dma = pltpu.SemaphoreType.DMA
    scratch = [
        pltpu.VMEM(w_query.shape, bf16),
        pltpu.VMEM(w_key.shape, bf16),
        pltpu.VMEM(w_value.shape, bf16),
        pltpu.VMEM((block, heads), bf16),
        pltpu.VMEM(cache_keys.shape, bf16),
        pltpu.VMEM(cache_values.shape, bf16),
        pltpu.VMEM((chunk_count, batch, heads, LANES), f32),
        pltpu.VMEM(w_out.shape, bf16),
        pltpu.VMEM(w_gate.shape, bf16),
        pltpu.VMEM(w_up.shape, bf16),
        pltpu.VMEM(w_down.shape, bf16),
        pltpu.VMEM((tp_count, ROWS, LANES), f32),
        pltpu.VMEM((kv_count, 3, ROWS, LANES), f32),
        pltpu.VMEM((tp_count, ROWS, LANES), f32),
        pltpu.VMEM((tp_count * 2 * ROWS, LANES), f32),
        pltpu.VMEM((tp_count, 2 * ROWS, LANES), f32),
        pltpu.VMEM((kv_count, 2 * ROWS, LANES), f32),
        pltpu.VMEM((2 * ROWS, LANES), f32),
        pltpu.VMEM((tp_count, ROWS, columns // 2), bf16),
        pltpu.VMEM((tp_count, ROWS, LANES), f32),
        pltpu.VMEM((kv_count, ROWS, LANES), f32),
        pltpu.VMEM((kv_count, ROWS, chunks[0][1] - chunks[0][0]), bf16),
        pltpu.VMEM((kv_count, ROWS, chunks[1][1] - chunks[1][0]), bf16),
        pltpu.VMEM((tp_count, ROWS, LANES), f32),
        pltpu.VMEM((tp_count, ROWS, LANES), f32),
        dma((10 + chunk_count,)),
        dma((5, tp_count - 1)),
        dma((5, tp_count - 1)),
        dma((5, kv_count - 1)),
        dma((5, kv_count - 1)),
    ]
    return pl.pallas_call(
        functools.partial(layer_kernel, kv_count, tp_count),
        out_shape=jax.ShapeDtypeStruct(tokens.shape, bf16),
        in_specs=[pl.BlockSpec(memory_space=pltpu.SMEM)] + [in_vmem] * 5 + [anywhere] * 11,
        out_specs=in_vmem,
        scratch_shapes=scratch,
        compiler_params=pltpu.CompilerParams(
            collective_id=0, has_side_effects=True, vmem_limit_bytes=60 * 1024 * 1024
        ),
        name="decode_layer",
    )(
        lengths,
        tokens,
        attn_gain.reshape(1, -1),
        mlp_gain.reshape(1, -1),
        forget_bias.reshape(1, -1),
        out_gain.reshape(-1, LANES),
        w_query,
        w_key,
        w_value,
        w_forget,
        cache_keys,
        cache_values,
        cache_decay,
        w_out,
        w_gate,
        w_up,
        w_down,
    )


def dispatch(kv_count, tp_count, *arrays):
    tokens, w_query, cache_keys, w_gate = arrays[0], arrays[3], arrays[8], arrays[14]
    fits = (
        tokens.shape[0] <= 3
        and tokens.shape[1] == LANES
        and w_query.shape[1] == 4 * HD
        and tp_count == ROWS
        and cache_keys.shape[2] % LANES == 0
        and w_gate.shape[1] % LANES == 0
    )
    if fits:
        return kernel_layer(kv_count, tp_count, *arrays)
    return body(*arrays)


def solution(mesh):
    placed = (
        P(None, ("kv", "tp")),
        P(),
        P(("kv", "tp")),
        P("kv", "tp"),
        P("kv", None),
        P("kv", None),
        P(),
        P(),
        P(None, None, ("kv", "tp")),
        P(None, None, ("kv", "tp")),
        P(None, None, ("kv", "tp")),
        P(),
        P("tp", "kv"),
        P(("kv", "tp")),
        P("kv", "tp"),
        P("kv", "tp"),
        P("tp", "kv"),
    )
    chosen = functools.partial(dispatch, mesh.shape["kv"], mesh.shape["tp"])
    return jax.shard_map(
        chosen, mesh=mesh, in_specs=placed, out_specs=P(None, ("kv", "tp")), check_vma=False
    )
```

```python
import functools

import jax
import jax.numpy as jnp
from jax import lax
from jax.experimental import pallas as pl
from jax.experimental.pallas import tpu as pltpu
from jax.sharding import PartitionSpec as P

QUERY_HEAD_COUNT = 32
HD = 64
KV_HEADS = 2


epsilon = 1e-06
masked_score = -1e30


def spread_rows(share, gain):
    scaled = (share.astype(jnp.float32) * gain).astype(jnp.bfloat16)
    squares = jnp.sum(jnp.square(share.astype(jnp.float32)), axis=1)
    row_block = lax.all_gather(scaled, "tp", axis=1, tiled=True)
    square_total = lax.psum(squares, ("kv", "tp"))
    return (row_block, square_total)


def body(
    tokens,
    lengths,
    attn_gain,
    w_query,
    w_key,
    w_value,
    w_forget,
    forget_bias,
    cache_keys,
    cache_values,
    cache_decay,
    out_gain,
    w_out,
    mlp_gain,
    w_gate,
    w_up,
    w_down,
):
    full_width = tokens.shape[1] * lax.axis_size("kv") * lax.axis_size("tp")
    kv_index = lax.axis_index("kv")
    tp_index = lax.axis_index("tp")
    row_block, square_total = spread_rows(tokens, attn_gain)
    block_rows = row_block.shape[1]
    forget_rows = lax.dynamic_slice_in_dim(w_forget, kv_index * block_rows, block_rows, 0)
    query_part = jnp.dot(row_block, w_query, preferred_element_type=jnp.float32)
    key_part = jnp.dot(row_block, w_key, preferred_element_type=jnp.float32)
    value_part = jnp.dot(row_block, w_value, preferred_element_type=jnp.float32)
    forget_part = jnp.dot(row_block, forget_rows, preferred_element_type=jnp.float32)
    query_sum, key_sum, value_sum, forget_sum = lax.psum(
        (query_part, key_part, value_part, forget_part), "kv"
    )
    first_rms = lax.rsqrt(square_total / full_width + epsilon)[:, None]
    query_local = (query_sum * first_rms).astype(jnp.bfloat16)
    key_new = (key_sum * first_rms).astype(jnp.bfloat16)
    value_new = (value_sum * first_rms).astype(jnp.bfloat16)
    log_gate = jax.nn.log_sigmoid(forget_sum * first_rms + forget_bias)
    query_all = lax.all_gather(query_local, "tp", axis=1, tiled=True)
    batch_rows, key_dims, span = cache_keys.shape
    groups = QUERY_HEAD_COUNT // KV_HEADS
    score_scale = HD ** (-0.5)
    query_grouped = query_all.reshape(batch_rows, KV_HEADS, groups, HD)
    keys_grouped = cache_keys.reshape(batch_rows, KV_HEADS, HD, span)
    values_grouped = cache_values.reshape(batch_rows, KV_HEADS, HD, span)
    scores = jnp.einsum(
        "bkgd,bkdj->bkgj", query_grouped, keys_grouped, preferred_element_type=jnp.float32
    ).reshape(batch_rows, QUERY_HEAD_COUNT, span)
    scores = scores * score_scale + cache_decay + log_gate[:, :, None]
    first_slot = (kv_index * lax.axis_size("tp") + tp_index) * span
    token_positions = first_slot + lax.iota(jnp.int32, span)
    is_live = (token_positions[None, :] < lengths[:, None])[:, None, :]
    scores = jnp.where(is_live, scores, masked_score)
    own_score = (
        jnp.einsum(
            "inpo,ino->inp",
            query_grouped,
            key_new.reshape(batch_rows, KV_HEADS, HD),
            preferred_element_type=jnp.float32,
        ).reshape(batch_rows, QUERY_HEAD_COUNT)
        * score_scale
    )
    local_top = jnp.maximum(jnp.max(scores, axis=2), own_score)
    head_count = w_out.shape[0] // HD
    head_start = tp_index * head_count
    score_top = lax.pmax(local_top, ("kv", "tp"))
    weights = jnp.where(is_live, jnp.exp(scores - score_top[:, :, None]), 0.0)
    weight_total = jnp.sum(weights, axis=2)
    rounded = weights.astype(jnp.bfloat16).reshape(batch_rows, KV_HEADS, groups, span)
    value_sums = jnp.einsum(
        "bkgj,bkdj->bkgd", rounded, values_grouped, preferred_element_type=jnp.float32
    ).reshape(batch_rows, QUERY_HEAD_COUNT, HD)
    weight_total, value_sums = (weight_total, value_sums)
    weight_total, value_sums = (
        lax.psum_scatter(weight_total, "tp", scatter_dimension=1, tiled=True),
        lax.psum_scatter(value_sums, "tp", scatter_dimension=1, tiled=True),
    )
    weight_total, value_sums = lax.psum((weight_total, value_sums), "kv")
    score_top = lax.dynamic_slice_in_dim(score_top, head_start, head_count, 1)
    own_here = lax.dynamic_slice_in_dim(own_score, head_start, head_count, 1)
    new_values = jnp.repeat(value_new.reshape(batch_rows, KV_HEADS, HD), groups, axis=1)
    new_values = lax.dynamic_slice_in_dim(new_values, head_start, head_count, 1).astype(jnp.float32)
    own_weight = jnp.exp(own_here - score_top)
    heads_out = (value_sums + own_weight[:, :, None] * new_values) / (weight_total + own_weight)[
        :, :, None
    ]
    head_gains = lax.dynamic_slice_in_dim(out_gain, head_start * HD, head_count * HD, 0).reshape(
        head_count, HD
    )
    normed = (
        heads_out
        * lax.rsqrt(jnp.mean(jnp.square(heads_out), axis=2, keepdims=True) + epsilon)
        * head_gains
    )
    normed = normed.astype(jnp.bfloat16).reshape(batch_rows, head_count * HD)
    attn_part = jnp.dot(normed, w_out, preferred_element_type=jnp.float32)
    attn_share = lax.psum_scatter(attn_part, "tp", scatter_dimension=1, tiled=True)
    residual = (tokens.astype(jnp.float32) + attn_share).astype(jnp.bfloat16)
    mlp_block, mlp_squares = spread_rows(residual, mlp_gain)
    gate_part = jnp.dot(mlp_block, w_gate, preferred_element_type=jnp.float32)
    up_part = jnp.dot(mlp_block, w_up, preferred_element_type=jnp.float32)
    gate_sum, up_sum = lax.psum((gate_part, up_part), "kv")
    second_rms = lax.rsqrt(mlp_squares / full_width + epsilon)[:, None]
    hidden = (jax.nn.silu(gate_sum * second_rms) * (up_sum * second_rms)).astype(jnp.bfloat16)
    down_part = jnp.dot(hidden, w_down, preferred_element_type=jnp.float32)
    mlp_share = lax.psum_scatter(down_part, "tp", scatter_dimension=1, tiled=True)
    return (residual.astype(jnp.float32) + mlp_share).astype(jnp.bfloat16)


LANES = 128
ROWS = 8
MESH = pl.DeviceIdType.MESH


def column_chunks(columns):
    first = (columns // LANES + 1) // 2 * LANES
    return ((0, first), (first, columns))


def exchange(buffer, mine, axis, count, send_sems, recv_sems, source=None):
    copies = []
    for step in range(1, count):
        partner = lax.rem(mine + step, count)
        copy = pltpu.make_async_remote_copy(
            src_ref=buffer.at[mine] if source is None else source(partner),
            dst_ref=buffer.at[mine],
            send_sem=send_sems.at[step - 1],
            recv_sem=recv_sems.at[step - 1],
            device_id={axis: partner},
            device_id_type=MESH,
        )
        copy.start()
        copies.append(copy)
    return copies


def arrive(copies):
    for copy in copies:
        copy.wait_recv()


SLOT = HD // 4


def tops_of(part):
    starts = [HD + i * SLOT for i in range(3)]
    return functools.reduce(jnp.add, [part[:, i : i + 1] for i in starts])


def totals_of(part):
    start = HD + 3 * SLOT
    return part[:, start : start + 1] + part[:, start + SLOT // 2 : start + SLOT // 2 + 1]


def merge_partials(buffer, count, lane):
    parts = [buffer[i].astype(jnp.float32) for i in range(count)]
    tops = [tops_of(part) for part in parts]
    top = functools.reduce(jnp.maximum, tops)
    total = functools.reduce(
        jnp.add, [jnp.exp(one - top) * part for one, part in zip(tops, parts)]
    )
    total = jnp.where((lane >= HD) & (lane < HD + 3 * SLOT), 0.0, total)
    return jnp.where((lane >= HD) & (lane < HD + SLOT), top, total)


def layer_kernel(
    kv_count,
    tp_count,
    lengths_hbm,
    tokens_hbm,
    attn_gain_hbm,
    mlp_gain_hbm,
    forget_bias_hbm,
    out_gain_hbm,
    w_query_hbm,
    w_key_hbm,
    w_value_hbm,
    w_forget_hbm,
    keys_hbm,
    values_hbm,
    decay_hbm,
    w_out_hbm,
    w_gate_hbm,
    w_up_hbm,
    w_down_hbm,
    out,
    lengths,
    tokens,
    attn_gain,
    forget_bias,
    out_gain,
    stage,
    w_query,
    w_key,
    w_value,
    w_forget,
    keys,
    values,
    decay,
    w_out,
    w_gate,
    w_up,
    w_down,
    token_buf,
    gain_buf,
    proj_buf,
    new_buf,
    query_wire,
    query_buf,
    part_rows,
    part_send,
    part_buf,
    merged_buf,
    normed_buf,
    attn_buf,
    residual_buf,
    square_buf,
    gate_buf0,
    gate_buf1,
    down_send,
    down_buf,
    local_sem,
    tp_send,
    tp_recv,
    kv_send,
    kv_recv,
):
    kv = lax.axis_index("kv")
    tp = lax.axis_index("tp")
    batch = tokens.shape[0]
    half = ROWS // 2
    width = tokens.shape[1] * kv_count * tp_count
    block = w_query.shape[0]
    span = keys.shape[2]
    f32, bf16 = jnp.float32, jnp.bfloat16

    loads = {}

    def load(name, source, target):
        copy = pltpu.make_async_copy(source, target, local_sem.at[len(loads)])
        copy.start()
        loads[name] = copy

    load("tokens", tokens_hbm, tokens)
    load("attn_gain", attn_gain_hbm, attn_gain)
    barrier = pltpu.get_barrier_semaphore()
    for step in range(1, tp_count):
        pl.semaphore_signal(
            barrier, inc=1, device_id={"tp": lax.rem(tp + step, tp_count)}, device_id_type=MESH
        )
    for step in range(1, kv_count):
        pl.semaphore_signal(
            barrier, inc=1, device_id={"kv": lax.rem(kv + step, kv_count)}, device_id_type=MESH
        )
    stage[...] = jnp.zeros(stage.shape, f32)
    load("mlp_gain", mlp_gain_hbm, gain_buf.at[tp])
    load("query", w_query_hbm, w_query)
    load("key", w_key_hbm, w_key)
    load("value", w_value_hbm, w_value)
    load("forget", w_forget_hbm.at[:, pl.ds(pl.multiple_of(kv * block, block), block)], w_forget)
    load("forget_bias", forget_bias_hbm, forget_bias)
    load("out_gain", out_gain_hbm, out_gain)
    load("lengths", lengths_hbm, lengths)
    loads["tokens"].wait()
    loads["attn_gain"].wait()
    own_tokens = tokens[...].astype(f32)
    stage[0:batch, :] = own_tokens * attn_gain[...]
    stage[half : half + batch, :] = own_tokens
    token_buf[tp] = stage[...].astype(bf16)
    pl.semaphore_wait(barrier, tp_count + kv_count - 2)

    pending = []

    def tp_exchange(index, buffer, source=None):
        copies = exchange(
            buffer, tp, "tp", tp_count, tp_send.at[index], tp_recv.at[index], source
        )
        pending.extend(copies)
        return copies

    def kv_exchange(index, buffer):
        copies = exchange(buffer, kv, "kv", kv_count, kv_send.at[index], kv_recv.at[index])
        pending.extend(copies)
        return copies

    token_copies = tp_exchange(0, token_buf)
    load("keys", keys_hbm, keys)
    for c in range(span // LANES):
        load("decay%d" % c, decay_hbm.at[:, :, pl.ds(c * LANES, LANES)], decay.at[c])
    load("values", values_hbm, values)
    load("out", w_out_hbm, w_out)
    load("gate", w_gate_hbm, w_gate)
    load("up", w_up_hbm, w_up)
    load("down", w_down_hbm, w_down)
    part_rows[...] = jnp.zeros(part_rows.shape, f32)

    arrive(token_copies)
    blocks = [token_buf[i] for i in range(tp_count)]
    scaled = jnp.concatenate(blocks, axis=1)
    token_rows = scaled.astype(f32)[half:]
    squares = jnp.sum(token_rows * token_rows, axis=1, keepdims=True)
    squares = jnp.concatenate([squares, squares], axis=0)
    loads["query"].wait()
    query = jnp.dot(scaled, w_query[...], preferred_element_type=f32)
    proj_buf[kv, 0] = jnp.concatenate([query[:half, :LANES], query[:half, LANES:]], axis=0)
    proj_buf[kv, 1] = jnp.broadcast_to(squares, (ROWS, LANES))
    proj_copies = kv_exchange(0, proj_buf)
    loads["key"].wait()
    key = jnp.dot(scaled, w_key[...], preferred_element_type=f32)
    loads["value"].wait()
    value = jnp.dot(scaled, w_value[...], preferred_element_type=f32)
    loads["forget"].wait()
    forget = lax.dot_general(
        scaled, w_forget[...], (((1,), (1,)), ((), ())), preferred_element_type=f32
    )
    new_buf[kv, 0] = jnp.concatenate([key[:half], value[:half]], axis=0)
    heads = forget.shape[1]
    new_buf[kv, 1, :, 0:heads] = forget
    new_buf[kv, 1, :, heads:LANES] = jnp.zeros((ROWS, LANES - heads), f32)
    new_copies = kv_exchange(5, new_buf)
    loads["mlp_gain"].wait()
    arrive(proj_copies)
    query_sum, square_sum = [
        functools.reduce(jnp.add, [proj_buf[i, piece] for i in range(kv_count)])
        for piece in range(2)
    ]
    rms = lax.rsqrt(square_sum[:, 0:1] / width + epsilon)
    rms_twice = jnp.concatenate([rms[:half], rms[:half]], axis=0)
    query_wire[tp] = (query_sum * rms_twice).astype(bf16)
    query_copies = tp_exchange(1, query_wire)
    gain_copies = tp_exchange(5, gain_buf)
    loads["forget_bias"].wait()
    loads["out_gain"].wait()
    loads["lengths"].wait()
    arrive(new_copies)
    new_sum, forget_sum = [
        functools.reduce(jnp.add, [new_buf[i, piece] for i in range(kv_count)])
        for piece in range(2)
    ]
    new_rows = (new_sum * rms_twice).astype(bf16).astype(f32)
    raw_gate = forget_sum[:, 0:heads] * rms + forget_bias[...]
    log_gate = jnp.minimum(raw_gate, 0.0) - jnp.log1p(jnp.exp(-jnp.abs(raw_gate)))

    lane = lax.broadcasted_iota(jnp.int32, (ROWS, LANES), 1)
    group_rows = heads // KV_HEADS
    row_id = lax.broadcasted_iota(jnp.int32, (heads, heads), 0)
    row_rest = row_id % group_rows
    head_of_row = (
        row_id // group_rows * group_rows + row_rest % (group_rows // 2) * 2
        + row_rest // (group_rows // 2)
    )
    head_pick = head_of_row == lax.broadcasted_iota(jnp.int32, (heads, heads), 1)
    slots = lax.broadcasted_iota(jnp.int32, (heads, span), 1)
    slots = slots + (kv * tp_count + tp) * span
    first_device = jnp.broadcast_to(kv * tp_count + tp, (heads, 1)) == 0
    score_scale = HD ** (-0.5)
    arrive(query_copies)
    query_buf[...] = query_wire[...].astype(f32)
    query_flat = query_buf.reshape(tp_count * ROWS, LANES)
    half_rows = group_rows // 2
    pairs = [(g, p) for g in range(KV_HEADS) for p in range(2)]
    loads["keys"].wait()
    loads["values"].wait()
    for c in range(span // LANES):
        loads["decay%d" % c].wait()
    for b in range(batch):
        pieces = []
        for g, p in pairs:
            rows = query_flat[pl.ds(g * half_rows * half + b, half_rows, stride=half), :]
            if p != g:
                rows = pltpu.roll(rows, HD, 1)
            pieces.append(jnp.where(lane // HD == g, rows, 0.0))
        queries = jnp.concatenate(pieces, axis=0)
        own = jnp.sum(queries * new_rows[b : b + 1, :], axis=1, keepdims=True) * score_scale
        scores = jnp.dot(queries.astype(bf16), keys[b], preferred_element_type=f32)
        faded = jnp.concatenate(
            [
                jnp.concatenate(
                    [
                        decay[c, b, pl.ds(g * group_rows + p, half_rows, stride=2), :]
                        for g, p in pairs
                    ],
                    axis=0,
                )
                for c in range(span // LANES)
            ],
            axis=1,
        )
        gate_rows = jnp.sum(
            jnp.where(head_pick, log_gate[b : b + 1, :], 0.0), axis=1, keepdims=True
        )
        live = slots < lengths[b]
        scores = jnp.where(live, scores * score_scale + faded + gate_rows, masked_score)
        top = jnp.max(scores, axis=1, keepdims=True)
        top = jnp.where(first_device, jnp.maximum(top, own), top)
        weights = jnp.where(live, jnp.exp(scores - top), 0.0)
        own_weight = jnp.where(first_device, jnp.exp(jnp.minimum(own - top, 0.0)), 0.0)
        total = jnp.sum(weights, axis=1, keepdims=True) + own_weight
        mixed = lax.dot_general(
            weights.astype(bf16),
            values[b],
            (((1,), (1,)), ((), ())),
            preferred_element_type=f32,
        )
        mixed = mixed + own_weight * new_rows[half + b : half + b + 1, :]
        for i, (g, p) in enumerate(pairs):
            rows = slice(i * half_rows, (i + 1) * half_rows)
            tile = mixed[rows]
            if g:
                tile = pltpu.roll(tile, HD, 1)
            rest = top[rows]
            for start in range(HD, HD + 3 * SLOT, SLOT):
                piece = rest.astype(bf16).astype(f32)
                tile = jnp.where(lane < start, tile, piece)
                rest = rest - piece
            high = total[rows].astype(bf16).astype(f32)
            tile = jnp.where(lane < HD + 3 * SLOT, tile, high)
            tile = jnp.where(lane < HD + 3 * SLOT + SLOT // 2, tile, total[rows] - high)
            part_rows[pl.ds(g * half_rows * ROWS + 2 * b + p, half_rows, stride=ROWS), :] = tile

    part_send[...] = part_rows[...].astype(bf16)

    def part_of(index):
        return pl.ds(pl.multiple_of(index * 2 * ROWS, 2 * ROWS), 2 * ROWS)

    part_copies = tp_exchange(2, part_buf, lambda partner: part_send.at[part_of(partner), :])
    part_buf[tp] = part_send[part_of(tp), :]
    lane2 = lax.broadcasted_iota(jnp.int32, (2 * ROWS, LANES), 1)
    row2 = lax.broadcasted_iota(jnp.int32, (2 * ROWS, LANES), 0)
    gain_row = lax.broadcasted_iota(jnp.int32, out_gain.shape, 0)
    gain_tiles = []
    for j in range(2):
        gain = jnp.sum(
            jnp.where(gain_row == 2 * tp + j, out_gain[...], 0.0), axis=0, keepdims=True
        )
        gain = jnp.broadcast_to(gain, (ROWS, LANES))
        gain_tiles.append(jnp.where(row2[:ROWS] % 2 == 0, gain, pltpu.roll(gain, HD, 1)))
    gains = jnp.concatenate(gain_tiles, axis=0)
    arrive(part_copies)
    merged_buf[kv] = merge_partials(part_buf, tp_count, lane2)
    arrive(kv_exchange(1, merged_buf))
    merged = merge_partials(merged_buf, kv_count, lane2)
    total = totals_of(merged)
    total = jnp.where(row2[:, 0:1] % ROWS < 2 * batch, total, 1.0)
    heads_out = jnp.where(lane2 < HD, merged / total, 0.0)
    mean = jnp.sum(heads_out * heads_out, axis=1, keepdims=True) / HD
    normed_buf[...] = heads_out * lax.rsqrt(mean + epsilon) * gains
    columns = []
    for j in range(2):
        even = normed_buf[pl.ds(j * ROWS, half, stride=2), :]
        odd = normed_buf[pl.ds(j * ROWS + 1, half, stride=2), :]
        columns.append(jnp.where(lane[:half] < HD, even, pltpu.roll(odd, HD, 1)))
    normed = jnp.concatenate(columns, axis=1).astype(bf16)

    loads["out"].wait()
    attn = jnp.dot(normed, w_out[...], preferred_element_type=f32)
    middle = attn.shape[1] // 2
    attn_buf[tp] = jnp.concatenate([attn[:, :middle], attn[:, middle:]], axis=0).astype(bf16)
    arrive(tp_exchange(3, attn_buf))
    attn = functools.reduce(jnp.add, [attn_buf[i].astype(f32) for i in range(tp_count)])
    attn = jnp.concatenate([attn[:half], attn[half:]], axis=1)
    residual = (token_rows + attn).astype(bf16).astype(f32)
    squares = jnp.sum(residual * residual, axis=1, keepdims=True)
    square_buf[kv] = jnp.broadcast_to(
        jnp.concatenate([squares, squares], axis=0), (ROWS, LANES)
    )
    square_copies = kv_exchange(2, square_buf)
    for i in range(tp_count):
        residual_buf[i, 0:half, :] = residual[:, i * LANES : (i + 1) * LANES]
    arrive(gain_copies)
    gain_rows = jnp.concatenate([gain_buf[i] for i in range(tp_count)], axis=1)
    scaled = (residual * gain_rows).astype(bf16)

    loads["gate"].wait()
    loads["up"].wait()
    chunks = column_chunks(w_gate.shape[1])
    gate_bufs = (gate_buf0, gate_buf1)
    gate_copies = []
    for index, (begin, end) in enumerate(chunks):
        gate = jnp.dot(scaled, w_gate[:, begin:end], preferred_element_type=f32)
        up = jnp.dot(scaled, w_up[:, begin:end], preferred_element_type=f32)
        gate_bufs[index][kv] = jnp.concatenate([gate, up], axis=0).astype(bf16)
        gate_copies.append(kv_exchange(3 + index, gate_bufs[index]))
    arrive(square_copies)
    squares = functools.reduce(jnp.add, [square_buf[i] for i in range(kv_count)])
    rms = lax.rsqrt(squares[:half, 0:1] / width + epsilon)
    loads["down"].wait()
    down = jnp.zeros((half, w_down.shape[1]), f32)
    for index, (begin, end) in enumerate(chunks):
        arrive(gate_copies[index])
        both = functools.reduce(
            jnp.add, [gate_bufs[index][i].astype(f32) for i in range(kv_count)]
        )
        gate, up = both[:half] * rms, both[half:] * rms
        hidden = (gate / (1.0 + jnp.exp(-gate)) * up).astype(bf16)
        down = down + jnp.dot(hidden, w_down[begin:end, :], preferred_element_type=f32)
    for i in range(tp_count):
        down_send[i] = down[:, i * LANES : (i + 1) * LANES]
    down_copies = tp_exchange(4, down_buf, lambda partner: down_send.at[partner])
    down_buf[tp] = down_send[tp]
    arrive(down_copies)
    share = functools.reduce(jnp.add, [down_buf[i] for i in range(tp_count)])
    final = residual_buf[tp][0:batch] + share[0:batch]
    out[...] = final.astype(bf16)
    for copy in pending:
        copy.wait_send()


def kernel_layer(
    kv_count,
    tp_count,
    tokens,
    lengths,
    attn_gain,
    w_query,
    w_key,
    w_value,
    w_forget,
    forget_bias,
    cache_keys,
    cache_values,
    cache_decay,
    out_gain,
    w_out,
    mlp_gain,
    w_gate,
    w_up,
    w_down,
):
    f32, bf16 = jnp.float32, jnp.bfloat16
    batch, _, span = cache_keys.shape
    heads = w_forget.shape[1]
    block = w_query.shape[0]
    columns = w_out.shape[1]
    chunks = column_chunks(w_gate.shape[1])
    in_vmem = pl.BlockSpec(memory_space=pltpu.VMEM)
    anywhere = pl.BlockSpec(memory_space=pl.ANY)
    chunk_count = span // LANES
    dma = pltpu.SemaphoreType.DMA
    half = ROWS // 2
    scratch = [
        pltpu.SMEM(lengths.shape, jnp.int32),
        pltpu.VMEM(tokens.shape, bf16),
        pltpu.VMEM((1, LANES), f32),
        pltpu.VMEM((1, heads), f32),
        pltpu.VMEM((out_gain.shape[0] // LANES, LANES), f32),
        pltpu.VMEM((ROWS, LANES), f32),
        pltpu.VMEM(w_query.shape, bf16),
        pltpu.VMEM(w_key.shape, bf16),
        pltpu.VMEM(w_value.shape, bf16),
        pltpu.VMEM((heads, block), bf16),
        pltpu.VMEM(cache_keys.shape, bf16),
        pltpu.VMEM(cache_values.shape, bf16),
        pltpu.VMEM((chunk_count, batch, heads, LANES), f32),
        pltpu.VMEM(w_out.shape, bf16),
        pltpu.VMEM(w_gate.shape, bf16),
        pltpu.VMEM(w_up.shape, bf16),
        pltpu.VMEM(w_down.shape, bf16),
        pltpu.VMEM((tp_count, ROWS, LANES), bf16),
        pltpu.VMEM((tp_count, 1, LANES), f32),
        pltpu.VMEM((kv_count, 2, ROWS, LANES), f32),
        pltpu.VMEM((kv_count, 2, ROWS, LANES), f32),
        pltpu.VMEM((tp_count, ROWS, LANES), bf16),
        pltpu.VMEM((tp_count, ROWS, LANES), f32),
        pltpu.VMEM((tp_count * 2 * ROWS, LANES), f32),
        pltpu.VMEM((tp_count * 2 * ROWS, LANES), bf16),
        pltpu.VMEM((tp_count, 2 * ROWS, LANES), bf16),
        pltpu.VMEM((kv_count, 2 * ROWS, LANES), f32),
        pltpu.VMEM((2 * ROWS, LANES), f32),
        pltpu.VMEM((tp_count, ROWS, columns // 2), bf16),
        pltpu.VMEM((tp_count, ROWS, LANES), f32),
        pltpu.VMEM((kv_count, ROWS, LANES), f32),
        pltpu.VMEM((kv_count, ROWS, chunks[0][1] - chunks[0][0]), bf16),
        pltpu.VMEM((kv_count, ROWS, chunks[1][1] - chunks[1][0]), bf16),
        pltpu.VMEM((tp_count, half, LANES), f32),
        pltpu.VMEM((tp_count, half, LANES), f32),
        dma((16 + chunk_count,)),
        dma((6, tp_count - 1)),
        dma((6, tp_count - 1)),
        dma((6, kv_count - 1)),
        dma((6, kv_count - 1)),
    ]
    return pl.pallas_call(
        functools.partial(layer_kernel, kv_count, tp_count),
        out_shape=pltpu.VMEM(tokens.shape, bf16),
        in_specs=[anywhere] * 17,
        out_specs=in_vmem,
        scratch_shapes=scratch,
        compiler_params=pltpu.CompilerParams(
            collective_id=0, has_side_effects=True, vmem_limit_bytes=60 * 1024 * 1024
        ),
        name="decode_layer",
    )(
        lengths,
        tokens,
        attn_gain.reshape(1, -1),
        mlp_gain.reshape(1, -1),
        forget_bias.reshape(1, -1),
        out_gain.reshape(-1, LANES),
        w_query,
        w_key,
        w_value,
        w_forget.T,
        cache_keys,
        cache_values,
        cache_decay,
        w_out,
        w_gate,
        w_up,
        w_down,
    )


def dispatch(kv_count, tp_count, *arrays):
    tokens, w_query, cache_keys, w_gate = arrays[0], arrays[3], arrays[8], arrays[14]
    fits = (
        tokens.shape[0] <= 3
        and tokens.shape[1] == LANES
        and w_query.shape[1] == 4 * HD
        and tp_count == ROWS
        and cache_keys.shape[2] % LANES == 0
        and w_gate.shape[1] % LANES == 0
    )
    if fits:
        return kernel_layer(kv_count, tp_count, *arrays)
    return body(*arrays)


def solution(mesh):
    placed = (
        P(None, ("kv", "tp")),
        P(),
        P(("kv", "tp")),
        P("kv", "tp"),
        P("kv", None),
        P("kv", None),
        P(),
        P(),
        P(None, None, ("kv", "tp")),
        P(None, None, ("kv", "tp")),
        P(None, None, ("kv", "tp")),
        P(),
        P("tp", "kv"),
        P(("kv", "tp")),
        P("kv", "tp"),
        P("kv", "tp"),
        P("tp", "kv"),
    )
    chosen = functools.partial(dispatch, mesh.shape["kv"], mesh.shape["tp"])
    return jax.shard_map(
        chosen, mesh=mesh, in_specs=placed, out_specs=P(None, ("kv", "tp")), check_vma=False
    )
```
